32 devices in a mesh: fs: 16 (over z, y, x), tp: 2 (over core).
Axes of the slice: x: 2, y: 2, z: 4, core: 2. Of those that a mesh axis runs over, the one named last changes fastest.
Arguments:
- saved_inputs: bfloat16 [12288, 2048], P('fs'), may hold values from -6 to 6
- cotangents: bfloat16 [3, 12288, 1024], P(None, 'fs', 'tp'), may hold values from -0.0546875 to 0.0546875
- left_roots: float32 [3, 2048, 2048], P(None, 'fs'), may hold values from -1 to 2
- right_roots: float32 [3, 1024, 128], P(None, 'tp'), may hold values from -1 to 2
- moments: float32 [3, 2048, 1024], P(None, 'fs', 'tp'), may hold values from -125 to 125
- masters: float32 [3, 2048, 1024], P(None, 'fs', 'tp'), may hold values from -3 to 3
Outputs:
- direction: float32 [3, 2048, 1024], P(None, 'fs', 'tp')
- moments_new: float32 [3, 2048, 1024], P(None, 'fs', 'tp')
- copies: bfloat16 [3, 2048, 1024], P(None, None, 'tp')
The draws below stay inside these ranges and needn't reach their ends.
All inputs are finite; a program needn't handle non-finite values.
Results may differ from the reference program's by a relative error of at most 0.002.
Values may be sent and summed in bfloat16 or wider, within the bound.
A program may use at most 64 MiB of HBM per device.

```python
import math
import jax
import jax.numpy as jnp
from jax import lax

D = 2048
SBW = 1024
RB = 128
TOKENS = 12288


def draw_left_roots(key, part):
    key_main = jax.random.fold_in(key, 11)
    raw_values = jax.random.normal(key_main, (3, D, D), jnp.float32)
    spread = 0.5 / math.sqrt(D)
    symmetric = (raw_values + jnp.transpose(raw_values, (0, 2, 1))) * (spread / math.sqrt(2.0))
    return (symmetric + jnp.eye(D, dtype=jnp.float32)[None]).astype(jnp.float32)


def draw_right_roots(key, part):
    key_main = jax.random.fold_in(key, 23)
    block_count = SBW // RB
    raw_values = jax.random.normal(key_main, (3, block_count, RB, RB), jnp.float32)
    spread = 0.5 / math.sqrt(RB)
    symmetric = (raw_values + jnp.transpose(raw_values, (0, 1, 3, 2))) * (spread / math.sqrt(2.0))
    blocks = symmetric + jnp.eye(RB, dtype=jnp.float32)[None, None]
    return blocks.reshape(3, SBW, RB).astype(jnp.float32)


def draw_moments(key, part):
    key_noise = jax.random.fold_in(key, 31)
    key_rows = jax.random.fold_in(key, 37)
    key_cols = jax.random.fold_in(key, 41)
    row_pos = jnp.arange(D, dtype=jnp.float32)[None, :, None] / D
    col_pos = jnp.arange(SBW, dtype=jnp.float32)[None, None, :] / SBW
    row_scale = 10.0 ** (0.5 * row_pos + 0.5 * jax.random.uniform(key_rows, (3, D, 1), jnp.float32))
    col_scale = 10.0 ** (0.5 * col_pos + 0.5 * jax.random.uniform(key_cols, (3, 1, SBW), jnp.float32))
    raw_values = jnp.clip(jax.random.normal(key_noise, (3, D, SBW), jnp.float32), -4.0, 4.0)
    return 0.3 * raw_values * row_scale * col_scale


def spiked(drawn, key, source, target, parts, factor):
    owner, partner = [(jnp.arange(drawn.shape[axis_at]) // (drawn.shape[axis_at] // parts)).reshape([-1 if axis == axis_at else 1 for axis in range(drawn.ndim)]) for axis_at in (source, target)]
    chosen = jax.random.permutation(key, parts)[partner]
    strong = (owner == chosen) | (owner == (partner + parts // 2) % parts)
    return jnp.where(strong, factor * drawn, drawn)


def level_of(stream_key, extent, shards, smallest, largest):
    gain, own = 1.0, jax.random.fold_in(stream_key, 6)
    for position, parts in shards:
        heights = jnp.exp(jax.random.uniform(jax.random.fold_in(own, position), (parts,), jnp.float32, smallest / len(shards), largest / len(shards)))
        gain = gain * jnp.repeat(heights, extent[position] // parts).reshape([-1 if axis == position else 1 for axis in range(len(extent))])
    return gain


def gaussian(rng, extent, scale, reach, cuts=(), kind=jnp.bfloat16):
    values = jax.random.normal(rng, extent, jnp.float32) * scale
    if len(cuts) > 0:
        values = level_of(rng, extent, cuts, -0.22, 0.18) * values
    return jnp.clip(values, min=-reach, max=reach).astype(kind)


def heavy_noise(key, extent, width, most, pieces, heavy, kind=jnp.bfloat16):
    array = width * jax.random.normal(key, extent, jnp.float32)
    if pieces:
        array = array * level_of(key, extent, pieces, -0.22, 0.18)
    return jnp.clip(spiked(array, jax.random.fold_in(key, 3), *heavy), -most, most).astype(kind)


def setup_inputs(seed: int = 0) -> dict:
    seeds = jax.random.split(jax.random.key(seed), 7)
    saved_inputs = heavy_noise(seeds[0], (TOKENS, D), 1.0, 6.0, ((0, 16),), (0, 1, 16, 2.0))
    cotangents = gaussian(seeds[1], (3, TOKENS, SBW), (TOKENS ** -0.5), 0.0546875, ((1, 16), (2, 2)))
    left_roots = draw_left_roots(jax.random.fold_in(seeds[6], 71), 0)
    right_roots = draw_right_roots(jax.random.fold_in(seeds[6], 71), 0)
    moments = draw_moments(jax.random.fold_in(seeds[6], 71), 0)
    masters = gaussian(seeds[5], (3, D, SBW), 0.5, 3.0, ((1, 16), (2, 2)), jnp.float32)
    return {"saved_inputs": saved_inputs, "cotangents": cotangents, "left_roots": left_roots, "right_roots": right_roots, "moments": moments, "masters": masters}


momentum_decay = 0.9
step_rate = 0.1
eps_value = 1e-06

def reference(saved_inputs, cotangents, left_roots, right_roots, moments, masters):
    gradients = jnp.einsum('td,mtc->mdc', saved_inputs.astype(jnp.float32), cotangents.astype(jnp.float32))
    left_done = jnp.einsum('mde,mec->mdc', left_roots, gradients, precision=lax.Precision.HIGHEST)
    block_count = SBW // RB
    right_blocks = right_roots.reshape(3, block_count, RB, RB)
    right_done = jnp.einsum('mdbi,mbij->mdbj', left_done.reshape(3, D, block_count, RB), right_blocks, precision=lax.Precision.HIGHEST).reshape(3, D, SBW)
    moments_new = momentum_decay * moments + right_done
    meansq = lax.optimization_barrier(jnp.mean(moments_new * moments_new, axis=(1, 2), keepdims=True))
    direction = moments_new * lax.rsqrt(meansq + eps_value)
    copies = (masters - step_rate * direction).astype(jnp.bfloat16)
    return (direction, moments_new, copies)
```

```python
import functools

import jax
import jax.numpy as jnp
from jax import lax
from jax.experimental import pallas as pl
from jax.experimental.pallas import tpu as pltpu
from jax.sharding import PartitionSpec as P

RB = 128
momentum_decay = 0.9
step_rate = 0.1
eps_value = 1e-06
MESH = pl.DeviceIdType.MESH
F32 = jnp.float32
BF16 = jnp.bfloat16


def step_kernel(
    n, tpn, x_ref, c_ref, l_ref, r_ref, mom_ref, mas_ref, dir_ref, mnew_ref, out_ref,
    gp, r1, t1, r2, t2, r3, acc, gf, cf, own, st1, st2, mid,
    s_first, s_second, s_third, a_first, a_second, a_third, q_row, q_col, out_sem,
):
    g = n // 4
    count, rows, cols = mom_ref.shape
    depth = x_ref.shape[1]
    half = rows // 2
    me = lax.axis_index("fs")
    tp = lax.axis_index("tp")
    z, y, x = me // 4, (me // 2) % 2, me % 2
    y_peer, x_peer = me + 2 - 4 * y, me + 1 - 2 * x
    near = ((y, x, y_peer, x_peer), (x, y, x_peer, y_peer))

    def block(ref, m, h, zi, p, q):
        return ref.at[m, zi, p, q, h] if h == 0 else ref.at[m, zi, q, p, h]

    def pair(ref, m, h, zi, p):
        return ref.at[m, zi, p, :, h] if h == 0 else ref.at[m, zi, :, p, h]

    def remote(src, dst, sems, at, peer, axis="fs"):
        return pltpu.make_async_remote_copy(
            src_ref=src, dst_ref=dst, send_sem=sems.at[(0,) + at], recv_sem=sems.at[(1,) + at],
            device_id={axis: peer}, device_id_type=MESH,
        )

    def loop(low, high, body):
        def step(i, carry):
            body(i)
            return carry

        lax.fori_loop(low, high, step, 0)

    def around(d):
        return (z + d) % g

    def first(m, h, zi):
        p, _, peer, _ = near[h]
        return remote(pair(gp, m, h, zi, 1 - p), r1.at[m, h, zi], s_first, (m, h, zi), peer)

    def second(m, h, zi):
        return remote(t1.at[m, h, zi], r2.at[m, h, zi], s_second, (m, h, zi), near[h][3])

    def third(m, h, d):
        return remote(t2.at[m, h, d], r3.at[m, h, d], s_third, (m, h, d), around(d) * 4 + y * 2 + x)

    def value(m, h, zi, q):
        p = near[h][0]
        return block(gp, m, h, zi, p, q)[...].astype(F32) + r1[m, h, zi, q].astype(F32)

    def stage_partial(m):
        wide = 4 * rows

        def body(zi):
            part = lax.dot_general(
                x_ref[:, pl.ds(pl.multiple_of(zi * wide, wide), wide)], c_ref[m],
                (((0,), (0,)), ((), ())), preferred_element_type=F32,
            )
            gp[m, zi] = part.astype(BF16).reshape(2, 2, 2, half, cols)
            first(m, 0, zi).start()
            first(m, 1, zi).start()

        loop(0, g, body)

    def stage_second(m):
        def body(zi):
            for h in range(2):
                q = near[h][1]
                first(m, h, zi).wait_recv()
                t1[m, h, zi] = value(m, h, zi, 1 - q).astype(BF16)
                second(m, h, zi).start()

        loop(0, g, body)

    def stage_third(m):
        def reduced(h, zi):
            second(m, h, zi).wait_recv()
            return value(m, h, zi, near[h][1]) + r2[m, h, zi].astype(F32)

        def body(d):
            for h in range(2):
                t2[m, h, d] = reduced(h, around(d)).astype(BF16)
                third(m, h, d).start()

        loop(1, g, body)
        for h in range(2):
            acc[h] = reduced(h, z)

    def spread(k, buf, m, h, d):
        slot = block(buf, m, h, z, *near[h][:2])
        return remote(slot, slot, a_first, (k, m, h, d), around(d) * 4 + y * 2 + x)

    def across(k, buf, m, h, d):
        slot = block(buf, m, h, around(g - d), *near[h][:2])
        return remote(slot, slot, a_second, (k, m, h, d), near[h][3])

    def last(k, buf, m, h, d):
        slot = pair(buf, m, h, around(g - d), near[h][0])
        return remote(slot, slot, a_third, (k, m, h, d), near[h][2])

    def landed_spread(k, buf, m, h, d):
        slot = block(buf, m, h, around(g - d), *near[h][:2])
        return remote(slot, slot, a_first, (k, m, h, d), around(g - d) * 4 + y * 2 + x)

    def landed_across(k, buf, m, h, d):
        p, q, _, peer = near[h]
        slot = block(buf, m, h, around(g - d), p, 1 - q)
        return remote(slot, slot, a_second, (k, m, h, d), peer)

    def landed_last(k, buf, m, h, d):
        p, _, peer, _ = near[h]
        slot = pair(buf, m, h, around(g - d), 1 - p)
        return remote(slot, slot, a_third, (k, m, h, d), peer)

    def gather_start(k, buf, m):
        for h in range(2):
            across(k, buf, m, h, 0).start()

        def body(d):
            for h in range(2):
                spread(k, buf, m, h, d).start()

        loop(1, g, body)

    def gather_across(k, buf, m):
        def body(d):
            for h in range(2):
                landed_spread(k, buf, m, h, d).wait_recv()
                across(k, buf, m, h, d).start()

        loop(1, g, body)

    def gather_last(k, buf, m):
        def body(d):
            for h in range(2):
                landed_across(k, buf, m, h, d).wait_recv()
                last(k, buf, m, h, d).start()

        loop(0, g, body)

    def gather_wait(k, buf, m):
        def body(d):
            for h in range(2):
                landed_last(k, buf, m, h, d).wait_recv()

        loop(0, g, body)

    def stage_rows(m):
        def body(d):
            for h in range(2):
                third(m, h, d).wait_recv()
                acc[h] += r3[m, h, d].astype(F32)

        loop(1, g, body)
        for h in range(2):
            gf[m, z, y, x, h] = acc[h].astype(BF16)
        gather_start(0, gf, m)

    def row_sum(m, d):
        return remote(own.at[m], st1.at[m, d], q_row, (m, d), (me + d) % n)

    def col_sum(m, d):
        return remote(mid.at[m], st2.at[m, d], q_col, (m, d), (tp + d) % tpn, "tp")

    def stage_product(m):
        gather_wait(0, gf, m)
        roots = l_ref[m]
        high = roots.astype(BF16)
        low = (roots - high.astype(F32)).astype(BF16)
        both = jnp.dot(
            jnp.concatenate([high, low], axis=0), gf[m].reshape(depth, cols),
            preferred_element_type=F32,
        )
        left = both[:rows] + both[rows:]
        tile = jnp.zeros((8, RB), F32)
        for b in range(cols // RB):
            at = slice(b * RB, (b + 1) * RB)
            right = jnp.dot(
                left[:, at], r_ref[m, at, :], precision=lax.Precision.HIGHEST,
                preferred_element_type=F32,
            )
            new = momentum_decay * mom_ref[m, :, at] + right
            mnew_ref[m, :, at] = new
            tile += jnp.sum((new * new).reshape(rows // 8, 8, RB), axis=0)
        own[m] = tile
        loop(1, n, lambda d: row_sum(m, d).start())

    def stage_sum(m):
        loop(1, n, lambda d: row_sum(m, d).wait_recv())
        mid[m] = own[m] + jnp.sum(st1[m, 1:], axis=0)
        loop(1, tpn, lambda d: col_sum(m, d).start())

    def stage_copies(m):
        loop(1, tpn, lambda d: col_sum(m, d).wait_recv())
        tile = mid[m] + jnp.sum(st2[m, 1:], axis=0)
        total = jnp.sum(jnp.sum(tile, axis=1, keepdims=True), axis=0, keepdims=True)
        scale = lax.rsqrt(total / (depth * cols * tpn) + eps_value)
        direction = mnew_ref[m] * scale
        dir_ref[m] = direction
        cf[m, z, y, x] = (mas_ref[m] - step_rate * direction).astype(BF16).reshape(2, half, cols)
        gather_start(1, cf, m)

    def put(m):
        return pltpu.make_async_copy(cf.at[m], out_ref.at[m], out_sem.at[m])

    def stage_put(m):
        gather_wait(1, cf, m)
        put(m).start()

    stages = (
        stage_partial, stage_second, stage_third, stage_rows,
        functools.partial(gather_across, 0, gf), functools.partial(gather_last, 0, gf),
        stage_product, stage_sum, stage_copies,
        functools.partial(gather_across, 1, cf), functools.partial(gather_last, 1, cf), stage_put,
    )
    for t in range(len(stages) + count - 1):
        if t < count:
            stages[0](t)
        for m in range(min(t, count)):
            if t - m < len(stages):
                stages[t - m](m)

    for m in range(count):
        put(m).wait()

        def sent(d):
            for h in range(2):
                first(m, h, d).wait_send()
                second(m, h, d).wait_send()
                for k, buf in ((0, gf), (1, cf)):
                    across(k, buf, m, h, d).wait_send()
                    last(k, buf, m, h, d).wait_send()

        def sent_far(d):
            for h in range(2):
                third(m, h, d).wait_send()
                for k, buf in ((0, gf), (1, cf)):
                    spread(k, buf, m, h, d).wait_send()

        loop(0, g, sent)
        loop(1, g, sent_far)
        loop(1, n, lambda d: row_sum(m, d).wait_send())
        loop(1, tpn, lambda d: col_sum(m, d).wait_send())


def on_device(n, tpn, saved_inputs, cotangents, left_roots, right_roots, moments, masters):
    g = n // 4
    count, rows, cols = moments.shape
    depth = saved_inputs.shape[1]
    half = rows // 2
    vmem = pl.BlockSpec(memory_space=pltpu.VMEM)
    grid_shape = (count, g, 2, 2, 2, half, cols)
    dma = pltpu.SemaphoreType.DMA
    direction, moments_new, copies = pl.pallas_call(
        functools.partial(step_kernel, n, tpn),
        out_shape=(
            jax.ShapeDtypeStruct(moments.shape, F32),
            jax.ShapeDtypeStruct(moments.shape, F32),
            jax.ShapeDtypeStruct(grid_shape, BF16),
        ),
        in_specs=[vmem] * 6,
        out_specs=(vmem, vmem, pl.BlockSpec(memory_space=pl.ANY)),
        scratch_shapes=[
            pltpu.VMEM(grid_shape, BF16),
            pltpu.VMEM((count, 2, g, 2, half, cols), BF16),
            pltpu.VMEM((count, 2, g, half, cols), BF16),
            pltpu.VMEM((count, 2, g, half, cols), BF16),
            pltpu.VMEM((count, 2, g, half, cols), BF16),
            pltpu.VMEM((count, 2, g, half, cols), BF16),
            pltpu.VMEM((2, half, cols), F32),
            pltpu.VMEM(grid_shape, BF16),
            pltpu.VMEM(grid_shape, BF16),
            pltpu.VMEM((count, 8, RB), F32),
            pltpu.VMEM((count, n, 8, RB), F32),
            pltpu.VMEM((count, tpn, 8, RB), F32),
            pltpu.VMEM((count, 8, RB), F32),
            dma((2, count, 2, g)), dma((2, count, 2, g)), dma((2, count, 2, g)),
            dma((2, 2, count, 2, g)), dma((2, 2, count, 2, g)), dma((2, 2, count, 2, g)),
            dma((2, count, n)), dma((2, count, tpn)), dma((count,)),
        ],
        compiler_params=pltpu.CompilerParams(
            has_side_effects=True, vmem_limit_bytes=64000 * 1024
        ),
        name="step",
    )(saved_inputs, cotangents, left_roots, right_roots, moments, masters)
    return direction, moments_new, copies.reshape(count, depth, cols)


def solution(mesh):
    placed = (
        P("fs", None),
        P(None, "fs", "tp"),
        P(None, "fs", None),
        P(None, "tp", None),
        P(None, "fs", "tp"),
        P(None, "fs", "tp"),
    )
    return jax.shard_map(
        functools.partial(on_device, mesh.shape["fs"], mesh.shape["tp"]),
        mesh=mesh,
        in_specs=placed,
        out_specs=(P(None, "fs", "tp"), P(None, "fs", "tp"), P(None, None, "tp")),
        check_vma=False,
    )
```

```python
import functools

import jax
import jax.numpy as jnp
from jax import lax
from jax.experimental import pallas as pl
from jax.experimental.pallas import tpu as pltpu
from jax.sharding import PartitionSpec as P

RB = 128
momentum_decay = 0.9
step_rate = 0.1
eps_value = 1e-06
MESH = pl.DeviceIdType.MESH
F32 = jnp.float32
BF16 = jnp.bfloat16


def step_kernel(
    n, tpn, x_in, c_in, l_in, r_in, mom_in, mas_in, dir_ref, mnew_ref, cf,
    x_ref, c_ref, l_ref, r_ref, mom_ref, mas_ref,
    gp, r1, t1, r2, t2, r3, acc, t2b, r3b, accb, gf, own, st1, st2, mid,
    s_first, s_second, s_third, a_first, a_second, a_third, a_fourth, q_row, q_col,
    x_sem, c_sem, in_sem,
):
    g = n // 4
    count, rows, cols = mom_ref.shape
    depth = x_ref.shape[1]
    half = rows // 2
    wide = 4 * rows
    far_first = -1
    me = lax.axis_index("fs")
    tp = lax.axis_index("tp")
    z, y, x = me // 4, (me // 2) % 2, me % 2
    y_peer, x_peer = me + 2 - 4 * y, me + 1 - 2 * x
    near = ((y, x, y_peer, x_peer), (x, y, x_peer, y_peer))

    def block(ref, m, h, zi, p, q):
        return ref.at[m, zi, p, q, h] if h == 0 else ref.at[m, zi, q, p, h]

    def pair(ref, m, h, zi, p):
        return ref.at[m, zi, p, :, h] if h == 0 else ref.at[m, zi, :, p, h]

    def remote(src, dst, sems, at, peer, axis="fs"):
        return pltpu.make_async_remote_copy(
            src_ref=src, dst_ref=dst, send_sem=sems.at[(0,) + at], recv_sem=sems.at[(1,) + at],
            device_id={axis: peer}, device_id_type=MESH,
        )

    def loop(low, high, body):
        def step(i, carry):
            body(i)
            return carry

        lax.fori_loop(low, high, step, 0)

    def around(d):
        return (z + d) % g

    def first(m, h, zi):
        p, _, peer, _ = near[h]
        return remote(pair(gp, m, h, zi, 1 - p), r1.at[m, h, zi], s_first, (m, h, zi), peer)

    def second(m, h, zi):
        return remote(t1.at[m, h, zi], r2.at[m, h, zi], s_second, (m, h, zi), near[h][3])

    def third(m, h, d):
        return remote(t2.at[m, h, d], r3.at[m, h, d], s_third, (m, h, d), around(d) * 4 + y * 2 + x)

    def value(m, h, zi, q):
        p = near[h][0]
        return block(gp, m, h, zi, p, q)[...].astype(F32) + r1[m, h, zi, q].astype(F32)

    def load_x(zi):
        at = pl.ds(pl.multiple_of(zi * wide, wide), wide)
        return pltpu.make_async_copy(x_in.at[:, at], x_ref.at[:, at], x_sem.at[zi])

    def load_c(m):
        return pltpu.make_async_copy(c_in.at[m], c_ref.at[m], c_sem.at[m])

    later = (
        pltpu.make_async_copy(l_in, l_ref, in_sem.at[0]),
        pltpu.make_async_copy(r_in, r_ref, in_sem.at[1]),
        pltpu.make_async_copy(mom_in, mom_ref, in_sem.at[2]),
        pltpu.make_async_copy(mas_in, mas_ref, in_sem.at[3]),
    )
    load_c(0).start()
    loop(0, g, lambda zi: load_x(zi).start())
    for m in range(1, count):
        load_c(m).start()
    for copy in later:
        copy.start()

    def stage_partial(m):
        load_c(m).wait()

        def body(zi):
            if m == 0:
                load_x(zi).wait()
            part = lax.dot_general(
                x_ref[:, pl.ds(pl.multiple_of(zi * wide, wide), wide)], c_ref[m],
                (((0,), (0,)), ((), ())), preferred_element_type=F32,
            )
            gp[m, zi] = part.astype(BF16).reshape(2, 2, 2, half, cols)
            first(m, 0, zi).start()
            first(m, 1, zi).start()

        loop(0, g, body)

    def third_wide(h, d):
        peer = around(d) * 4 + y * 2 + x
        return remote(t2b.at[h, d], r3b.at[h, d], s_third, (far_first, h, d), peer)

    def stage_second_far(m):
        def summed(h, zi):
            first(m, h, zi).wait_recv()
            kept = pair(gp, m, h, zi, near[h][0])[...].astype(F32)
            return kept + r1[m, h, zi].astype(F32)

        def body(d):
            for h in range(2):
                t2b[h, d] = summed(h, around(d)).astype(BF16)
                third_wide(h, d).start()

        loop(1, g, body)
        for h in range(2):
            accb[h] = summed(h, z)

    def stage_third_far(m):
        def body(d):
            for h in range(2):
                third_wide(h, d).wait_recv()
                accb[h] += r3b[h, d].astype(F32)

        loop(1, g, body)
        for h in range(2):
            t1[m, h, 0] = accb[h, 1 - near[h][1]].astype(BF16)
            second(m, h, 0).start()

    def stage_second(m):
        if m == far_first:
            return stage_second_far(m)

        def body(zi):
            for h in range(2):
                q = near[h][1]
                first(m, h, zi).wait_recv()
                t1[m, h, zi] = value(m, h, zi, 1 - q).astype(BF16)
                second(m, h, zi).start()

        loop(0, g, body)

    def stage_third(m):
        if m == far_first:
            return stage_third_far(m)

        def reduced(h, zi):
            second(m, h, zi).wait_recv()
            return value(m, h, zi, near[h][1]) + r2[m, h, zi].astype(F32)

        def body(d):
            for h in range(2):
                t2[m, h, d] = reduced(h, around(d)).astype(BF16)
                third(m, h, d).start()

        loop(1, g, body)
        for h in range(2):
            acc[h] = reduced(h, z)

    def spread(k, buf, m, h, d):
        slot = block(buf, m, h, z, *near[h][:2])
        return remote(slot, slot, a_first, (k, m, h, d), around(d) * 4 + y * 2 + x)

    def across(k, buf, m, h, d):
        slot = block(buf, m, h, around(g - d), *near[h][:2])
        return remote(slot, slot, a_second, (k, m, h, d), near[h][3])

    def last(k, buf, m, h, d):
        slot = pair(buf, m, h, around(g - d), near[h][0])
        return remote(slot, slot, a_third, (k, m, h, d), near[h][2])

    def landed_spread(k, buf, m, h, d):
        slot = block(buf, m, h, around(g - d), *near[h][:2])
        return remote(slot, slot, a_first, (k, m, h, d), around(g - d) * 4 + y * 2 + x)

    def landed_across(k, buf, m, h, d):
        p, q, _, peer = near[h]
        slot = block(buf, m, h, around(g - d), p, 1 - q)
        return remote(slot, slot, a_second, (k, m, h, d), peer)

    def landed_last(k, buf, m, h, d):
        p, _, peer, _ = near[h]
        slot = pair(buf, m, h, around(g - d), 1 - p)
        return remote(slot, slot, a_third, (k, m, h, d), peer)

    def gather_start(k, buf, m):
        for h in range(2):
            across(k, buf, m, h, 0).start()

        def body(d):
            for h in range(2):
                spread(k, buf, m, h, d).start()

        loop(1, g, body)

    def spread_near(k, buf, m, h, d):
        p, q, _, _ = near[h]
        slot = block(buf, m, h, z, p, 1 - q)
        return remote(slot, slot, a_fourth, (k, h, d), around(d) * 4 + y * 2 + x)

    def landed_spread_near(k, buf, m, h, d):
        p, q, _, _ = near[h]
        slot = block(buf, m, h, around(g - d), p, 1 - q)
        return remote(slot, slot, a_fourth, (k, h, d), around(g - d) * 4 + y * 2 + x)

    def gather_across_far(k, buf, m):
        for h in range(2):
            landed_across(k, buf, m, h, 0).wait_recv()

        def body(d):
            for h in range(2):
                spread_near(k, buf, m, h, d).start()

        loop(1, g, body)

    def gather_last_far(k, buf, m):
        for h in range(2):
            last(k, buf, m, h, 0).start()

        def body(d):
            for h in range(2):
                landed_spread(k, buf, m, h, d).wait_recv()
                landed_spread_near(k, buf, m, h, d).wait_recv()
                last(k, buf, m, h, d).start()

        loop(1, g, body)

    def gather_across(k, buf, m):
        if m == far_first:
            return gather_across_far(k, buf, m)

        def body(d):
            for h in range(2):
                landed_spread(k, buf, m, h, d).wait_recv()
                across(k, buf, m, h, d).start()

        loop(1, g, body)

    def gather_last(k, buf, m):
        if m == far_first:
            return gather_last_far(k, buf, m)

        def body(d):
            for h in range(2):
                landed_across(k, buf, m, h, d).wait_recv()
                last(k, buf, m, h, d).start()

        loop(0, g, body)

    def gather_wait(k, buf, m):
        def body(d):
            for h in range(2):
                landed_last(k, buf, m, h, d).wait_recv()

        loop(0, g, body)

    def stage_rows(m):
        def body(d):
            for h in range(2):
                third(m, h, d).wait_recv()
                acc[h] += r3[m, h, d].astype(F32)

        if m != far_first:
            loop(1, g, body)
        for h in range(2):
            if m == far_first:
                second(m, h, 0).wait_recv()
                gf[m, z, y, x, h] = (accb[h, near[h][1]] + r2[m, h, 0].astype(F32)).astype(BF16)
            else:
                gf[m, z, y, x, h] = acc[h].astype(BF16)
        gather_start(0, gf, m)

    def row_sum(m, d):
        return remote(own.at[m], st1.at[m, d], q_row, (m, d), (me + d) % n)

    def col_sum(m, d):
        return remote(mid.at[m], st2.at[m, d], q_col, (m, d), (tp + d) % tpn, "tp")

    def stage_product(m):
        gather_wait(0, gf, m)
        if m == 0:
            for copy in later:
                copy.wait()
        roots = l_ref[m]
        high = roots.astype(BF16)
        low = (roots - high.astype(F32)).astype(BF16)
        both = jnp.dot(
            jnp.concatenate([high, low], axis=0), gf[m].reshape(depth, cols),
            preferred_element_type=F32,
        )
        left = both[:rows] + both[rows:]
        tile = jnp.zeros((8, RB), F32)
        for b in range(cols // RB):
            at = slice(b * RB, (b + 1) * RB)
            right = jnp.dot(
                left[:, at], r_ref[m, at, :], precision=lax.Precision.HIGHEST,
                preferred_element_type=F32,
            )
            new = momentum_decay * mom_ref[m, :, at] + right
            mnew_ref[m, :, at] = new
            tile += jnp.sum((new * new).reshape(rows // 8, 8, RB), axis=0)
        own[m] = tile
        loop(1, n, lambda d: row_sum(m, d).start())

    def stage_sum(m):
        loop(1, n, lambda d: row_sum(m, d).wait_recv())
        mid[m] = own[m] + jnp.sum(st1[m, 1:], axis=0)
        loop(1, tpn, lambda d: col_sum(m, d).start())

    def stage_copies(m):
        loop(1, tpn, lambda d: col_sum(m, d).wait_recv())
        tile = mid[m] + jnp.sum(st2[m, 1:], axis=0)
        total = jnp.sum(jnp.sum(tile, axis=1, keepdims=True), axis=0, keepdims=True)
        scale = lax.rsqrt(total / (depth * cols * tpn) + eps_value)
        direction = mnew_ref[m] * scale
        dir_ref[m] = direction
        cf[m, z, y, x] = (mas_ref[m] - step_rate * direction).astype(BF16).reshape(2, half, cols)
        gather_start(1, cf, m)

    stages = (
        stage_partial, stage_second, stage_third, stage_rows,
        functools.partial(gather_across, 0, gf), functools.partial(gather_last, 0, gf),
        stage_product, stage_sum, stage_copies,
        functools.partial(gather_across, 1, cf), functools.partial(gather_last, 1, cf),
        functools.partial(gather_wait, 1, cf),
    )
    skew = 2
    order = sorted((i + skew * m, i > 0, m, i) for m in range(count) for i in range(len(stages)))
    for _, _, m, i in order:
        stages[i](m)

    for m in range(count):
        far = m == far_first

        def sent(d):
            for h in range(2):
                first(m, h, d).wait_send()
                for k, buf in ((0, gf), (1, cf)):
                    last(k, buf, m, h, d).wait_send()

        def sent_second(d):
            for h in range(2):
                second(m, h, d).wait_send()
                for k, buf in ((0, gf), (1, cf)):
                    across(k, buf, m, h, d).wait_send()

        def sent_far(d):
            for h in range(2):
                (third_wide(h, d) if far else third(m, h, d)).wait_send()
                for k, buf in ((0, gf), (1, cf)):
                    spread(k, buf, m, h, d).wait_send()
                    if far:
                        spread_near(k, buf, m, h, d).wait_send()

        loop(0, g, sent)
        loop(0, 1 if far else g, sent_second)
        loop(1, g, sent_far)
        loop(1, n, lambda d: row_sum(m, d).wait_send())
        loop(1, tpn, lambda d: col_sum(m, d).wait_send())


def put_kernel(dir_ref, mnew_ref, cf, dir_out, mnew_out, cf_out, sem):
    copies = [
        pltpu.make_async_copy(src, dst, sem.at[i])
        for i, (src, dst) in enumerate(((cf, cf_out), (dir_ref, dir_out), (mnew_ref, mnew_out)))
    ]
    for copy in copies:
        copy.start()
    for copy in copies:
        copy.wait()


def on_device(n, tpn, saved_inputs, cotangents, left_roots, right_roots, moments, masters):
    g = n // 4
    count, rows, cols = moments.shape
    depth = saved_inputs.shape[1]
    half = rows // 2
    vmem = pl.BlockSpec(memory_space=pltpu.VMEM)
    anywhere = pl.BlockSpec(memory_space=pl.ANY)
    grid_shape = (count, g, 2, 2, 2, half, cols)
    dma = pltpu.SemaphoreType.DMA
    direction, moments_new, copies = pl.pallas_call(
        functools.partial(step_kernel, n, tpn),
        out_shape=(
            pltpu.VMEM(moments.shape, F32),
            pltpu.VMEM(moments.shape, F32),
            pltpu.VMEM(grid_shape, BF16),
        ),
        in_specs=[anywhere] * 6,
        out_specs=(vmem, vmem, vmem),
        scratch_shapes=[
            pltpu.VMEM(saved_inputs.shape, BF16),
            pltpu.VMEM(cotangents.shape, BF16),
            pltpu.VMEM(left_roots.shape, F32),
            pltpu.VMEM(right_roots.shape, F32),
            pltpu.VMEM(moments.shape, F32),
            pltpu.VMEM(masters.shape, F32),
            pltpu.VMEM(grid_shape, BF16),
            pltpu.VMEM((count, 2, g, 2, half, cols), BF16),
            pltpu.VMEM((count, 2, g, half, cols), BF16),
            pltpu.VMEM((count, 2, g, half, cols), BF16),
            pltpu.VMEM((count, 2, g, half, cols), BF16),
            pltpu.VMEM((count, 2, g, half, cols), BF16),
            pltpu.VMEM((2, half, cols), F32),
            pltpu.VMEM((2, g, 2, half, cols), BF16),
            pltpu.VMEM((2, g, 2, half, cols), BF16),
            pltpu.VMEM((2, 2, half, cols), F32),
            pltpu.VMEM(grid_shape, BF16),
            pltpu.VMEM((count, 8, RB), F32),
            pltpu.VMEM((count, n, 8, RB), F32),
            pltpu.VMEM((count, tpn, 8, RB), F32),
            pltpu.VMEM((count, 8, RB), F32),
            dma((2, count, 2, g)), dma((2, count, 2, g)), dma((2, count, 2, g)),
            dma((2, 2, count, 2, g)), dma((2, 2, count, 2, g)), dma((2, 2, count, 2, g)),
            dma((2, 2, 2, g)),
            dma((2, count, n)), dma((2, count, tpn)),
            dma((g,)), dma((count,)), dma((4,)),
        ],
        compiler_params=pltpu.CompilerParams(
            has_side_effects=True, vmem_limit_bytes=52000 * 1024
        ),
        name="step",
    )(saved_inputs, cotangents, left_roots, right_roots, moments, masters)
    direction, moments_new, copies = pl.pallas_call(
        put_kernel,
        out_shape=(
            jax.ShapeDtypeStruct(moments.shape, F32),
            jax.ShapeDtypeStruct(moments.shape, F32),
            jax.ShapeDtypeStruct(grid_shape, BF16),
        ),
        in_specs=[vmem] * 3,
        out_specs=(anywhere,) * 3,
        scratch_shapes=[dma((3,))],
        compiler_params=pltpu.CompilerParams(vmem_limit_bytes=4096 * 1024),
        name="put",
    )(direction, moments_new, copies)
    return direction, moments_new, copies.reshape(count, depth, cols)


def solution(mesh):
    placed = (
        P("fs", None),
        P(None, "fs", "tp"),
        P(None, "fs", None),
        P(None, "tp", None),
        P(None, "fs", "tp"),
        P(None, "fs", "tp"),
    )
    return jax.shard_map(
        functools.partial(on_device, mesh.shape["fs"], mesh.shape["tp"]),
        mesh=mesh,
        in_specs=placed,
        out_specs=(P(None, "fs", "tp"), P(None, "fs", "tp"), P(None, None, "tp")),
        check_vma=False,
    )
```
